32 devices in a mesh: ep: 8 (over z, x), tp: 4 (over y, core).
Axes of the slice: x: 2, y: 2, z: 4, core: 2. Of those that a mesh axis runs over, the one named last changes fastest.
Arguments:
- out_gate: bfloat16 [4096, 2048], P(('ep', 'tp')), may hold values from -6 to 6
- in_gate: bfloat16 [4096, 2048], P(('ep', 'tp')), may hold values from -6 to 6
- conv_input: bfloat16 [4096, 2048], P(('ep', 'tp')), may hold values from -6 to 6
- conv_taps: bfloat16 [3, 2048], replicated, may hold values from -3 to 3
- mixer_weight: bfloat16 [2048, 2048], P(None, 'tp'), may hold values from -0.125 to 0.125
- expert_input: bfloat16 [4096, 2048], P(('ep', 'tp')), may hold values from -6 to 6
- norm_gain: float32 [2048], replicated, may hold values from 0.1 to 1.9
- expert_gate: bfloat16 [8, 2048, 1024], P('ep', None, 'tp'), may hold values from -0.125 to 0.125
- expert_up: bfloat16 [8, 2048, 1024], P('ep', None, 'tp'), may hold values from -0.125 to 0.125
- expert_down: bfloat16 [8, 1024, 2048], P('ep', 'tp'), may hold values from -0.1875 to 0.1875
- expert_ids: int32 [4096, 2], P(('ep', 'tp')), may hold values from 0 to 7, all different within a row; in each aligned block of 128 rows (0 to 127, 128 to 255, ...) at most 64 rows name the same one
- route_weight: float32 [4096, 2], P(('ep', 'tp')), may hold values from 0.1 to 1
Outputs:
- mixer_out: bfloat16 [4096, 2048], P('ep', 'tp')
- experts_out: bfloat16 [4096, 2048], P(('ep', 'tp'))
The draws below stay inside these ranges and needn't reach their ends.
Inputs may be any that keep to these rules, and one draw needn't show every extreme that they name: `expert_ids`: each row names 2 different experts. Within the 128 rows of one device no expert is named by more than 64 rows, and in some devices' rows some expert is named by exactly 64.
All inputs are finite; a program needn't handle non-finite values.
Results may differ from the reference program's by a relative error of at most 0.011.
Values may be sent and summed in bfloat16 or wider, within the bound.
A program may use at most 128 MiB of HBM per device.

```python
import math
import jax
import jax.numpy as jnp
import numpy as np
from jax import lax

D = 2048
FF = 1024
TOP = 2
CONV = 3
SEQS = 1
TOK_DEV = 128
TOKENS = 4096
EXPERTS = 8
CAP = 64
N_TP = 4


def shard_levels(own_key, dims, cuts, smallest, largest):
    level = 1.0
    for dim, shards_of in cuts:
        heights = jax.random.uniform(jax.random.fold_in(jax.random.fold_in(own_key, 6), dim), (shards_of,), jnp.float32, smallest / len(cuts), largest / len(cuts))
        level = level * jnp.repeat(jnp.exp(heights), dims[dim] // shards_of).reshape((-1,) + (1,) * (len(dims) - 1 - dim))
    return level


def deal_out(key, own, number, rows, amount, top, most, slope):
    sequence = jax.random.permutation(key, amount)
    heavy_load, ordinary = load_shares(amount, rows * top, most, slope, True), load_shares(amount, rows * top, most, slope, False)
    places = jnp.arange(amount)

    def named(lengths, offset_by):
        used = int((lengths > 0).sum())
        fixed = max(1, used // 4)
        passed = fixed + (places - fixed + offset_by * (used - fixed)) % max(1, amount - fixed)
        return jnp.zeros((amount,), jnp.int32).at[sequence[jnp.where(places < fixed, places, passed)]].set(jnp.asarray(lengths, jnp.int32))

    lengths = jnp.where(number % 4 == 0, named(heavy_load, number // 4), named(ordinary, number - number // 4 - 1))
    mixed = jax.random.permutation(jax.random.fold_in(own, 3), amount)
    source_of, taker = mixed[0:amount // 2 * 2:2], mixed[1:amount // 2 * 2:2]
    slack = jnp.minimum(lengths[source_of] - 1, most - lengths[taker]) // 2
    slack = jnp.where((source_of == sequence[0]) | (taker == sequence[0]) | (lengths[taker] == 0), 0, jnp.maximum(slack, 0))
    passed = jax.random.randint(jax.random.fold_in(own, 4), (amount // 2,), 0, 1 << 20) % (slack + 1)
    lengths = lengths.at[source_of].add(-passed).at[taker].add(passed)
    members = jnp.searchsorted(jnp.cumsum(lengths), jnp.arange(rows * top), side="right").astype(jnp.int32)
    grid = members.reshape(top, rows).T
    grid = grid[jax.random.permutation(jax.random.fold_in(own, 1), rows)]
    offset_by = jax.random.randint(jax.random.fold_in(own, 2), (rows, 1), 0, top)
    return jnp.take_along_axis(grid, (jnp.arange(top)[None, :] + offset_by) % top, axis=1)


def load_shares(number_of, total, most, skew, full):
    loads = [(1 << 20) // math.isqrt(standing ** skew) + 1 for standing in range(1, number_of + 1)]
    largest = most if full else min(most, max(-(-total // number_of), total * loads[0] // sum(loads)))
    least = 1 if total - largest >= number_of - 1 else 0
    given, surplus = [largest] + [least] * (number_of - 1), total - largest - least * (number_of - 1)
    while surplus > 0:
        free = [i for i in range(1, number_of) if given[i] < largest] or [i for i in range(1, number_of) if given[i] < most]
        mass, left = sum([loads[i] for i in free]), surplus
        for i in free:
            addition = min(most - given[i], max(1, left * loads[i] // mass), surplus)
            given[i] = given[i] + addition
            surplus = surplus - addition
    return np.array(given)


def normal_values(key, extent, spread, most, pieces=(), held_as=jnp.bfloat16):
    array = spread * jax.random.normal(key, extent, jnp.float32)
    if pieces:
        array = array * shard_levels(key, extent, pieces, -0.22, 0.18)
    return jnp.clip(array, -most, most).astype(held_as)


def setup_inputs(seed: int = 0) -> dict:
    seeds = jax.random.split(jax.random.key(seed), 13)
    out_gate = normal_values(seeds[0], (TOKENS, D), 1.0, 6.0, ((0, 32),))
    in_gate = normal_values(seeds[1], (TOKENS, D), 1.0, 6.0, ((0, 32),))
    conv_input = normal_values(seeds[2], (TOKENS, D), 1.0, 6.0, ((0, 32),))
    conv_taps = normal_values(seeds[3], (CONV, D), 0.577, 3.0)
    mixer_weight = normal_values(seeds[4], (D, D), D ** -0.5, 0.125, ((1, 4),))
    expert_input = normal_values(seeds[5], (TOKENS, D), 1.0, 6.0, ((0, 32),))
    norm_gain = jnp.clip(1.0 + 0.18 * jax.random.normal(seeds[6], (D,), jnp.float32), 0.1, 1.9)
    expert_gate = normal_values(seeds[7], (EXPERTS, D, FF), D ** -0.5, 0.125, ((0, 8), (2, 4)))
    expert_up = normal_values(seeds[8], (EXPERTS, D, FF), D ** -0.5, 0.125, ((0, 8), (2, 4)))
    expert_down = normal_values(seeds[9], (EXPERTS, FF, D), FF ** -0.5, 0.1875, ((0, 8), (1, 4)))
    expert_ids_keys = jax.random.split(jax.random.fold_in(seeds[10], 1), TOKENS // TOK_DEV)
    expert_ids_turns = jax.random.permutation(jax.random.fold_in(seeds[10], 3), TOKENS // TOK_DEV)
    expert_ids = jax.vmap(lambda own, number: deal_out(jax.random.fold_in(seeds[10], 2), own, number, TOK_DEV, EXPERTS, TOP, CAP, 1))(expert_ids_keys, expert_ids_turns).reshape((TOKENS, TOP))
    route_weight = jnp.clip(jnp.exp(math.log(1.0) - 2.3025851 * jax.random.uniform(seeds[11], (TOKENS, TOP), jnp.float32) ** shard_levels(seeds[11], (TOKENS, TOP), ((0, 32),), -0.2, 0.2)), 0.1, 1.0)
    return {"out_gate": out_gate, "in_gate": in_gate, "conv_input": conv_input, "conv_taps": conv_taps, "mixer_weight": mixer_weight, "expert_input": expert_input, "norm_gain": norm_gain, "expert_gate": expert_gate, "expert_up": expert_up, "expert_down": expert_down, "expert_ids": expert_ids, "route_weight": route_weight}


norm_eps = 1e-06

def device_slots(route_ids, expert_count):
    flat_ids = route_ids.reshape(-1)
    member = (flat_ids[:, None] == jnp.arange(expert_count, dtype=jnp.int32)[None, :]).astype(jnp.int32)
    before = jnp.cumsum(member, axis=0) - member
    return lax.optimization_barrier(jnp.sum(before * member, axis=1)).astype(jnp.int32).reshape(route_ids.shape)

def short_conv(out_gate, in_gate, conv_input, conv_taps, mixer_weight):
    product = in_gate.astype(jnp.float32) * conv_input.astype(jnp.float32)
    seq_length = TOKENS // SEQS
    by_sequence = product.reshape(SEQS, seq_length, D)
    padded = jnp.pad(by_sequence, ((0, 0), (CONV - 1, 0), (0, 0)))
    tap_values = conv_taps.astype(jnp.float32)
    smoothed = sum((padded[:, tap_index:tap_index + seq_length] * tap_values[tap_index] for tap_index in range(CONV)))
    gated = (out_gate.astype(jnp.float32) * smoothed.reshape(TOKENS, D)).astype(jnp.bfloat16)
    return jnp.dot(gated, mixer_weight, preferred_element_type=jnp.float32).astype(jnp.bfloat16)

def routed_experts(expert_input, norm_gain, expert_gate, expert_up, expert_down, expert_ids, route_weight):
    wide_input = expert_input.astype(jnp.float32)
    inv_norm = lax.rsqrt(lax.optimization_barrier(jnp.mean(wide_input * wide_input, axis=1, keepdims=True)) + norm_eps)
    normed = (wide_input * inv_norm * norm_gain.astype(jnp.float32)).astype(jnp.bfloat16)
    devices = TOKENS // TOK_DEV
    block_ids = expert_ids.reshape(devices, TOK_DEV, TOP).astype(jnp.int32)

    def block_slots(route_ids):
        return device_slots(route_ids, EXPERTS)
    slot_rank = jax.vmap(block_slots)(block_ids)
    device_index = jnp.arange(devices, dtype=jnp.int32)[:, None, None]
    slot_index = (device_index * CAP + slot_rank).astype(jnp.int32)
    token_index = (device_index * TOK_DEV + jnp.arange(TOK_DEV, dtype=jnp.int32)[None, :, None] + jnp.zeros_like(slot_rank)).astype(jnp.int32)
    slot_table = jnp.zeros((EXPERTS, devices * CAP), jnp.int32).at[block_ids, slot_index].set(token_index)
    fourth = FF // N_TP

    def one_expert(operands):
        token_rows, w_gate, w_up, w_down = operands
        slot_rows = normed[token_rows]
        gate_proj = jnp.dot(slot_rows, w_gate, preferred_element_type=jnp.float32)
        up_proj = jnp.dot(slot_rows, w_up, preferred_element_type=jnp.float32)
        hidden = (jax.nn.silu(gate_proj) * up_proj).astype(jnp.bfloat16)
        running = jnp.zeros((slot_rows.shape[0], D), jnp.float32)
        for quarter in range(N_TP):
            partial_sum = jnp.dot(hidden[:, quarter * fourth:(quarter + 1) * fourth], w_down[quarter * fourth:(quarter + 1) * fourth], preferred_element_type=jnp.float32)
            running = running + lax.optimization_barrier(partial_sum.astype(jnp.bfloat16)).astype(jnp.float32)
        return running.astype(jnp.bfloat16)
    results = lax.map(one_expert, (slot_table, expert_gate, expert_up, expert_down))
    picked = results[block_ids, slot_index].reshape(TOKENS, TOP, D).astype(jnp.float32)
    route_share = route_weight / lax.optimization_barrier(jnp.sum(route_weight, axis=1, keepdims=True))
    return lax.optimization_barrier(jnp.sum(picked * route_share[:, :, None], axis=1)).astype(jnp.bfloat16)

def reference(out_gate, in_gate, conv_input, conv_taps, mixer_weight, expert_input, norm_gain, expert_gate, expert_up, expert_down, expert_ids, route_weight):
    mixer_out = short_conv(out_gate, in_gate, conv_input, conv_taps, mixer_weight)
    experts_out = routed_experts(expert_input, norm_gain, expert_gate, expert_up, expert_down, expert_ids, route_weight)
    return (mixer_out, experts_out)
```

```python
import functools

import jax
import jax.numpy as jnp
from jax import lax
from jax.experimental import pallas as pl
from jax.experimental.pallas import tpu as pltpu
from jax.sharding import PartitionSpec as P

CONV = 3
SEQS = 1


norm_eps = 1e-06


def from_behind(value, axis, steps):
    count = lax.axis_size(axis)
    first, last = (max(0, -steps), min(count, count - steps))
    return lax.ppermute(value, axis, [(source, source + steps) for source in range(first, last)])


def device_slots(route_ids, expert_count):
    flat_ids = route_ids.reshape(-1)
    member = (flat_ids[:, None] == jnp.arange(expert_count, dtype=jnp.int32)[None, :]).astype(
        jnp.int32
    )
    before = jnp.cumsum(member, axis=0) - member
    return jnp.sum(before * member, axis=1).reshape(route_ids.shape)


def fill_slots(row_data, route_ids, expert_count, slot_cap):
    top_count = route_ids.shape[1]
    position = (route_ids * slot_cap + device_slots(route_ids, expert_count)).reshape(-1)
    zeroed = jnp.zeros((expert_count * slot_cap, row_data.shape[1]), row_data.dtype)
    return zeroed.at[position].set(jnp.repeat(row_data, top_count, axis=0))


def expert_hidden(slot_rows, w_gate, w_up):
    gate_proj = jnp.dot(slot_rows, w_gate, preferred_element_type=jnp.float32)
    up_proj = jnp.dot(slot_rows, w_up, preferred_element_type=jnp.float32)
    return (jax.nn.silu(gate_proj) * up_proj).astype(jnp.bfloat16)


def local(
    out_gate,
    in_gate,
    conv_input,
    conv_taps,
    mixer_weight,
    expert_input,
    norm_gain,
    expert_gate,
    expert_up,
    expert_down,
    expert_ids,
    route_weight,
):
    row_count = in_gate.shape[0]
    tap_span = CONV - 1
    group_size = lax.axis_size("tp")
    product = in_gate.astype(jnp.float32) * conv_input.astype(jnp.float32)
    edge_product = from_behind(product[row_count - tap_span :], ("ep", "tp"), 1)
    seq_length = row_count * lax.axis_size("ep") * group_size // SEQS
    linear_index = lax.axis_index("ep") * group_size + lax.axis_index("tp")
    carry_over = jnp.where(linear_index * row_count % seq_length == 0, 0.0, 1.0).astype(jnp.float32)
    earlier = edge_product * carry_over
    padded = jnp.concatenate([earlier, product], axis=0)
    tap_values = conv_taps.astype(jnp.float32)
    smoothed = sum(
        (
            padded[tap_index : tap_index + row_count] * tap_values[tap_index]
            for tap_index in range(CONV)
        )
    )
    gated = (out_gate.astype(jnp.float32) * smoothed).astype(jnp.bfloat16)
    token_count = expert_input.shape[0]
    model_width = expert_input.shape[1]
    expert_count = lax.axis_size("ep")
    slot_cap = 4 * token_count // expert_count
    wide_input = expert_input.astype(jnp.float32)
    inv_norm = lax.rsqrt(jnp.mean(wide_input * wide_input, axis=1, keepdims=True) + norm_eps)
    normed = (wide_input * inv_norm * norm_gain).astype(jnp.bfloat16)
    w_gate = expert_gate[0]
    hidden_width = w_gate.shape[1]
    position = (expert_ids * slot_cap + device_slots(expert_ids, expert_count)).reshape(-1)
    whole_gate, whole_up, whole_down = (
        lax.all_gather(expert_gate, "tp", axis=2, tiled=True),
        lax.all_gather(expert_up, "tp", axis=2, tiled=True),
        lax.all_gather(expert_down, "tp", axis=1, tiled=True),
    )
    mixer_out = jnp.dot(
        lax.all_gather(gated, "tp", axis=0, tiled=True),
        mixer_weight,
        preferred_element_type=jnp.float32,
    ).astype(jnp.bfloat16)
    outgoing = fill_slots(normed, expert_ids, expert_count, slot_cap).reshape(
        expert_count, slot_cap, model_width
    )
    arrived = lax.all_to_all(outgoing, "ep", split_axis=0, concat_axis=0, tiled=True)
    hidden = expert_hidden(arrived.reshape(-1, model_width), whole_gate[0], whole_up[0])
    running = jnp.zeros((hidden.shape[0], model_width), jnp.float32)
    for quarter in range(group_size):
        partial_sum = jnp.dot(
            hidden[:, quarter * hidden_width : (quarter + 1) * hidden_width],
            whole_down[0, quarter * hidden_width : (quarter + 1) * hidden_width],
            preferred_element_type=jnp.float32,
        )
        running = running + lax.optimization_barrier(partial_sum.astype(jnp.bfloat16)).astype(
            jnp.float32
        )
    summed = running.astype(jnp.bfloat16)
    returned = lax.all_to_all(
        summed.reshape(expert_count, slot_cap, model_width),
        "ep",
        split_axis=0,
        concat_axis=0,
        tiled=True,
    )
    picked = returned.reshape(expert_count * slot_cap, model_width)[position]
    top_count = expert_ids.shape[1]
    picked = picked.reshape(token_count, top_count, model_width).astype(jnp.float32)
    route_share = route_weight / jnp.sum(route_weight, axis=1, keepdims=True)
    experts_out = jnp.sum(picked * route_share[:, :, None], axis=1).astype(jnp.bfloat16)
    return (mixer_out, experts_out)


MESH = pl.DeviceIdType.MESH
PIECES = 8
SPLITS = 4
EAGER = 3
BEHIND = 2


def fused_kernel(
    ep_size,
    tp_size,
    cap,
    x_hbm,
    gain_hbm,
    taps_hbm,
    ids_hbm,
    weight_hbm,
    og_hbm,
    ig_hbm,
    ci_hbm,
    mw_hbm,
    wg_hbm,
    wu_hbm,
    wd_hbm,
    mix_ref,
    out_ref,
    x_ref,
    gain_ref,
    taps_ref,
    ids_ref,
    weight_ref,
    og,
    ig,
    ci,
    mw,
    gates,
    ups,
    downs,
    xs,
    xr,
    hid,
    g_sum,
    u_sum,
    ys,
    yr,
    prod,
    gat,
    place,
    normed,
    summed,
    sums,
    info,
    their_info,
    picks,
    their_place,
    their_rows,
    local_sem,
    own_sem,
    y_send,
    y_recv,
    c_send,
    c_recv,
    f_send,
    f_recv,
    x_send,
    x_recv,
    r_send,
    r_recv,
    e_send,
    e_recv,
    g_send,
    g_recv,
    p_send,
    p_recv,
    m_send,
    m_recv,
    n_send,
    n_recv,
):
    f32, bf16 = jnp.float32, jnp.bfloat16
    ep, tp = lax.axis_index("ep"), lax.axis_index("tp")
    rows, width = x_ref.shape
    x_copies, og_copies = (2, 3, 4, 7), (5, 6)
    piece = width // PIECES
    depth = width // SPLITS
    part = wd_hbm.shape[0]
    tp_c = tp + 1 - 2 * lax.rem(tp, 2)
    tp_y = lax.rem(tp + 2, tp_size)
    line = ep * tp_size + tp
    count = ep_size * tp_size
    after, before = lax.rem(line + 1, count), lax.rem(line + count - 1, count)
    after_id = (after // tp_size, lax.rem(after, tp_size))
    before_id = (before // tp_size, lax.rem(before, tp_size))
    core_id, y_id = (ep, tp_c), (ep, tp_y)

    bits = [1 << b for b in range(ep_size.bit_length() - 1)]
    half = ep_size // 2

    def peer(k):
        return sum(lax.rem(ep // b + k // b, 2) * b for b in bits)

    barrier = pltpu.get_barrier_semaphore()
    partners = [(peer(k), tp) for k in range(1, half + 1)] + [core_id, y_id, after_id, before_id]
    for partner in partners:
        pl.semaphore_signal(barrier, inc=1, device_id=partner, device_id_type=MESH)

    stage = [
        pltpu.make_async_copy(s, d, local_sem.at[i])
        for i, (s, d) in enumerate(
            (
                (ig_hbm, ig),
                (ci_hbm, ci),
                (x_hbm, x_ref),
                (ids_hbm, ids_ref),
                (gain_hbm, gain_ref),
                (og_hbm, og),
                (taps_hbm, taps_ref),
                (weight_hbm, weight_ref),
                (mw_hbm, mw),
            )
        )
    ]
    for copy in stage:
        copy.start()

    def parts(owner):
        cut = [(wg_hbm, gates.at[owner])]
        for k in range(SPLITS):
            deep = pl.ds(k * depth, depth)
            cut.append((wu_hbm.at[deep], ups.at[owner, deep]))
        at = pl.ds(pl.multiple_of(owner * part, part), part)
        for j in range(PIECES):
            cut.append((wd_hbm.at[:, pl.ds(j * piece, piece)], downs.at[j, at]))
        return cut

    def remote(s, d, ss, rs, who):
        return pltpu.make_async_remote_copy(
            src_ref=s, dst_ref=d, send_sem=ss, recv_sem=rs, device_id=who, device_id_type=MESH
        )

    def taken(ref, sem):
        pltpu.make_async_copy(ref, ref, sem).wait()

    group = [0] * (1 + SPLITS) + [1] * PIECES
    held = (gates.at[0:2], gates.at[0])
    own = [pltpu.make_async_copy(s, d, own_sem.at[g]) for g, (s, d) in zip(group, parts(tp))]
    for copy in own:
        copy.start()
    head = 8
    strip = 256
    stage[0].wait()
    stage[1].wait()
    last = slice(rows - head, rows)
    prod[rows : rows + head, :] = ig[last, :].astype(f32) * ci[last, :].astype(f32)
    edge = remote(prod.at[rows : rows + head], prod.at[0:head], e_send, e_recv, after_id)
    to_y = [remote(s, d, y_send, y_recv.at[i], y_id) for i, (s, d) in enumerate(parts(tp))]
    to_c = [remote(s, d, c_send, c_recv.at[g], core_id) for g, (s, d) in zip(group, parts(tp))]
    pl.semaphore_wait(barrier, len(partners))
    edge.start()
    for copy in to_y + to_c:
        copy.start()

    def multiply(i, carry):
        c = pl.ds(pl.multiple_of(i * strip, strip), strip)
        first = slice(0, rows - head)
        prod[head:rows, c] = ig[first, c].astype(f32) * ci[first, c].astype(f32)
        return carry

    lax.fori_loop(0, width // strip, multiply, 0)

    for i in x_copies:
        stage[i].wait()
    ids_row = ids_ref[...]
    info[...] = jnp.concatenate(
        [ids_row.astype(f32), weight_ref[...], jnp.zeros((4, rows), f32)], axis=0
    )
    mirror = peer(half)
    tell = remote(info, their_info, m_send, m_recv, (mirror, tp))
    tell.start()
    lanes = place.shape[1]
    near = ep // half
    far = 1 - near
    turn = (far - near) * half
    ti = lax.broadcasted_iota(jnp.int32, (rows, rows), 0)
    tj = lax.broadcasted_iota(jnp.int32, (rows, rows), 1)
    upper = jnp.where(ti < tj, 1.0, 0.0).astype(bf16)
    expert_row = lax.broadcasted_iota(jnp.int32, place.shape, 0).astype(f32)

    def rank_rows(source, target):
        member = (source[0:1, :] == expert_row) | (source[1:2, :] == expert_row)
        member = jnp.where(member, 1.0, 0.0)
        rank = jnp.dot(member.astype(bf16), upper, preferred_element_type=f32)
        target[...] = jnp.where(member > 0.5, rank, -1.0)

    rank_rows(info, place)
    wide = x_ref[...].astype(f32)
    inv = lax.rsqrt(jnp.mean(wide * wide, axis=1, keepdims=True) + norm_eps)
    normed[...] = (wide * inv * gain_ref[...]).astype(bf16)
    slot = lax.broadcasted_iota(jnp.int32, (cap, rows), 0).astype(f32)
    across_rows = remote(normed, their_rows, n_send, n_recv, (mirror, tp))
    across_rows.start()

    def chosen(e, places, source):
        pick = jnp.where(places[pl.ds(e, 1), :] == slot, 1.0, 0.0).astype(bf16)
        return jnp.dot(pick, source[...], preferred_element_type=f32).astype(bf16)

    def send_rows(places, source, shift, which):
        def body(i, carry):
            e = peer(half - 1 - i)
            xs[e + shift] = chosen(e, places, source)
            remote(
                xs.at[e + shift],
                xr.at[ep + shift],
                x_send,
                x_recv.at[which],
                (e, tp),
            ).start()
            return carry

        lax.fori_loop(0, half - 1, body, 0)
        xr[ep + shift] = chosen(ep, places, source)

    send_rows(place, normed, 0, 0)

    for i in og_copies:
        stage[i].wait()
    edge.wait()

    @pl.when(line * rows % (rows * count // SEQS) == 0)
    def _():
        prod[0:head, :] = jnp.zeros((head, width), f32)

    def smooth(i, carry):
        c = pl.ds(pl.multiple_of(i * strip, strip), strip)
        taps = taps_ref[:, c].astype(f32)
        total = prod[head : head + rows, c] * taps[CONV - 1 : CONV]
        for j in range(CONV - 1):
            lo = head - (CONV - 1) + j
            total = total + prod[lo : lo + rows, c] * taps[j : j + 1]
        gat[tp, :, c] = (og[:, c].astype(f32) * total).astype(bf16)
        return carry

    lax.fori_loop(0, width // strip, smooth, 0)
    g_y = remote(gat.at[tp], gat.at[tp], g_send.at[0], g_recv.at[0], y_id)
    g_c = remote(gat.at[tp], gat.at[tp], g_send.at[1], g_recv.at[1], core_id)
    g_y.start()
    g_c.start()

    def mix(t):
        mix_ref[pl.ds(pl.multiple_of(t * rows, rows), rows), :] = jnp.dot(
            gat[t], mw[...], preferred_element_type=f32
        ).astype(bf16)

    stage[8].wait()
    g_c.wait_recv()

    def mix_two(i, carry):
        mix(2 * (tp // 2) + i)
        return carry

    lax.fori_loop(0, 2, mix_two, 0)

    lane = tj.astype(f32)
    lower = jnp.where(tj < ti, 1.0, 0.0).astype(bf16)
    slots = lax.broadcasted_iota(jnp.int32, (rows, half * cap), 1).astype(f32)
    first = (near * half).astype(f32)

    def column(row):
        return jnp.sum(jnp.where(ti == tj, row, 0.0), axis=1, keepdims=True)

    def route(source, target):
        named = [column(source[k : k + 1, :]) for k in range(2)]
        weight = [column(source[2 + k : 3 + k, :]) for k in range(2)]
        member = jnp.where((named[0] == lane) | (named[1] == lane), 1.0, 0.0).astype(bf16)
        ranks = jnp.dot(lower, member, preferred_element_type=f32)
        for k in range(2):
            rank = jnp.sum(jnp.where(lane == named[k], ranks, 0.0), axis=1, keepdims=True)
            at = (named[k] - first) * cap + rank
            picks[target, k] = jnp.where(slots == at, 1.0, 0.0).astype(bf16)
        return [weight[k] / (weight[0] + weight[1]) for k in range(2)]

    shares = [route(info, 0)]
    tell.wait()
    shares.append(route(their_info, 1))

    def weighted(j, target):
        block = yr[j, target].reshape(half * cap, piece)
        total = shares[target][0] * jnp.dot(picks[target, 0], block, preferred_element_type=f32)
        return total + shares[target][1] * jnp.dot(
            picks[target, 1], block, preferred_element_type=f32
        )

    rank_rows(their_info, their_place)
    across_rows.wait()
    send_rows(their_place, their_rows, turn, 1)

    dest_y = parts(tp_y)
    forward = [
        remote(d, d, f_send, f_recv.at[i], core_id) for i, (_, d) in enumerate(dest_y)
    ]

    def side_rows(side):
        return pl.ds(pl.multiple_of(side * (half * cap), half * cap), half * cap)

    def units(q):
        return pl.ds(pl.multiple_of(q * part, part), part)

    def gated_units(g, u):
        return (g / (1.0 + jnp.exp(-g)) * u).astype(bf16)

    def arrived(side):
        return xr[pl.ds(side * half, half)].reshape(half * cap, width)

    def hidden(q, side):
        x = arrived(side)
        g = jnp.dot(x, gates[q], preferred_element_type=f32)
        u = jnp.dot(x, ups[q], preferred_element_type=f32)
        hid[side_rows(side), units(q)] = gated_units(g, u)

    chip, chip_other = 2 * (tp // 2), 1 - 2 * lax.rem(tp, 2)
    taken(xr.at[0 : half - 1], x_recv.at[0])
    taken(held[0], own_sem.at[0])
    taken(held[0], c_recv.at[0])

    def hidden_chip(i, carry):
        hidden(chip + lax.rem(i, 2), near + (i // 2) * (far - near))

        @pl.when(i == 1)
        def _():
            to_y[0].wait_recv()
            forward[0].start()
            taken(xr.at[0 : half - 1], x_recv.at[1])

        return carry

    lax.fori_loop(0, 4, hidden_chip, 0)
    crossed = (tp_y, tp_y + chip_other)

    def gate_part(i):
        def body(side, carry):
            g_sum[i, side_rows(side), :] = jnp.dot(
                arrived(side), gates[crossed[i]], preferred_element_type=f32
            )
            return carry

        lax.fori_loop(0, 2, body, 0)

    def up_part(i, k):
        deep = slice(k * depth, (k + 1) * depth)

        def body(side, carry):
            at = side_rows(side)
            x = xr[pl.ds(side * half, half), :, deep].reshape(half * cap, depth)
            u = jnp.dot(x, ups[crossed[i], deep], preferred_element_type=f32)
            if k:
                u = u + u_sum[i, at, :]
            if k < SPLITS - 1:
                u_sum[i, at, :] = u
            else:
                hid[at, units(crossed[i])] = gated_units(g_sum[i, at, :], u)
            return carry

        lax.fori_loop(0, 2, body, 0)

    gate_part(0)
    forward[0].wait_recv()
    gate_part(1)
    for k in range(SPLITS):
        to_y[1 + k].wait_recv()
        forward[1 + k].start()
        if k:
            forward[k].wait_recv()
            up_part(1, k - 1)
        up_part(0, k)
    forward[SPLITS].wait_recv()
    up_part(1, SPLITS - 1)

    mine = ep - near * half

    def give_back(j, kind, s):
        return remote(
            ys.at[j, s + kind * turn],
            yr.at[j, kind, mine],
            r_send,
            r_recv.at[j, kind],
            (s, tp),
        )

    def send_all(j, kind):
        def body(k, carry):
            give_back(j, kind, peer(half - 1 - k)).start()
            return carry

        lax.fori_loop(0, half - 1, body, 0)

    def wait_all(j, kind):
        taken(yr.at[j, kind, 0 : half - 1], r_recv.at[j, kind])

    across_half = [
        remote(summed.at[j], sums.at[j], p_send, p_recv.at[j], (mirror, tp))
        for j in range(PIECES)
    ]

    def relay(j):
        wait_all(j, 1)
        summed[j] = weighted(j, 1).astype(bf16)
        across_half[j].start()

    def down(j, side):
        total = jnp.dot(hid[side_rows(side), :], downs[j], preferred_element_type=f32)
        ys[j, pl.ds(side * half, half)] = total.astype(bf16).reshape(half, cap, piece)

    def finish(j):
        wait_all(j, 0)
        across_half[j].wait_recv()
        total = weighted(j, 0) + sums[j].astype(f32)
        out_ref[:, j * piece : (j + 1) * piece] = total.astype(bf16)

    taken(held[1], own_sem.at[1])
    taken(held[1], c_recv.at[1])
    for j in range(PIECES):
        m = 1 + SPLITS + j
        to_y[m].wait_recv()
        forward[m].start()
        if j >= BEHIND:
            relay(j - BEHIND)
        forward[m].wait_recv()
        down(j, far)
        yr[j, 1, mine] = ys[j, mirror]
        send_all(j, 1)
        down(j, near)
        yr[j, 0, mine] = ys[j, ep]
        if j < EAGER:
            send_all(j, 0)

    late = list(range(EAGER, PIECES))
    for j in range(PIECES - BEHIND, PIECES):
        for i in late[:2]:
            send_all(i, 0)
        late = late[2:]
        relay(j)
    for i in late:
        send_all(i, 0)

    g_y.wait_recv()
    g_f = remote(gat.at[tp_y], gat.at[tp_y], g_send.at[2], g_recv.at[2], core_id)
    g_f.start()
    mix(tp_y)
    g_f.wait_recv()
    mix(tp_y + chip_other)

    for j in range(PIECES):
        finish(j)

    for sem in (y_send, c_send, f_send):
        taken(gates.at[0:3], sem)
    taken(xr.at[0 : 2 * (half - 1)], x_send)
    taken(xr.at[0 : 2 * (half - 1)], r_send)
    taken(summed, p_send)
    for copy in [g_y, g_c, g_f]:
        copy.wait_send()


def place_kernel(mix_ref, out_ref, mix_hbm, out_hbm, sem):
    copies = [
        pltpu.make_async_copy(mix_ref, mix_hbm, sem.at[0]),
        pltpu.make_async_copy(out_ref, out_hbm, sem.at[1]),
    ]
    for copy in copies:
        copy.start()
    for copy in copies:
        copy.wait()


def placed(mix, out):
    vmem, hbm = pl.BlockSpec(memory_space=pltpu.VMEM), pl.BlockSpec(memory_space=pltpu.HBM)
    return pl.pallas_call(
        place_kernel,
        out_shape=tuple(jax.ShapeDtypeStruct(a.shape, a.dtype) for a in (mix, out)),
        in_specs=[vmem, vmem],
        out_specs=(hbm, hbm),
        scratch_shapes=[pltpu.SemaphoreType.DMA((2,))],
    )(mix, out)


def fused(
    out_gate,
    in_gate,
    conv_input,
    conv_taps,
    mixer_weight,
    expert_input,
    norm_gain,
    expert_gate,
    expert_up,
    expert_down,
    expert_ids,
    route_weight,
):
    ep_size, tp_size = lax.axis_size("ep"), lax.axis_size("tp")
    rows, width = expert_input.shape
    cap = 4 * rows // ep_size
    part = expert_gate.shape[2]
    columns = mixer_weight.shape[1]
    bf16, f32 = jnp.bfloat16, jnp.float32
    vmem, hbm = pl.BlockSpec(memory_space=pltpu.VMEM), pl.BlockSpec(memory_space=pltpu.HBM)
    dma = pltpu.SemaphoreType.DMA
    piece = width // PIECES
    blocks = 1 + SPLITS + PIECES
    mix, out = pl.pallas_call(
        functools.partial(fused_kernel, ep_size, tp_size, cap),
        out_shape=(
            pltpu.VMEM((rows * tp_size, columns), bf16),
            pltpu.VMEM((rows, width), bf16),
        ),
        in_specs=[hbm] * 12,
        out_specs=(vmem, vmem),
        scratch_shapes=[
            pltpu.VMEM((rows, width), bf16),
            pltpu.VMEM((1, width), f32),
            pltpu.VMEM(conv_taps.shape, bf16),
            pltpu.VMEM((expert_ids.shape[1], rows), jnp.int32),
            pltpu.VMEM((expert_ids.shape[1], rows), f32),
            pltpu.VMEM((rows, width), bf16),
            pltpu.VMEM((rows, width), bf16),
            pltpu.VMEM((rows, width), bf16),
            pltpu.VMEM(mixer_weight.shape, bf16),
            pltpu.VMEM((tp_size, width, part), bf16),
            pltpu.VMEM((tp_size, width, part), bf16),
            pltpu.VMEM((PIECES, tp_size * part, piece), bf16),
            pltpu.VMEM((ep_size, cap, width), bf16),
            pltpu.VMEM((ep_size, cap, width), bf16),
            pltpu.VMEM((ep_size * cap, tp_size * part), bf16),
            pltpu.VMEM((2, ep_size * cap, part), f32),
            pltpu.VMEM((2, ep_size * cap, part), f32),
            pltpu.VMEM((PIECES, ep_size, cap, piece), bf16),
            pltpu.VMEM((PIECES, 2, ep_size // 2, cap, piece), bf16),
            pltpu.VMEM((rows + 8, width), f32),
            pltpu.VMEM((tp_size, rows, width), bf16),
            pltpu.VMEM((max(8, ep_size), rows), f32),
            pltpu.VMEM((rows, width), bf16),
            pltpu.VMEM((PIECES, rows, piece), bf16),
            pltpu.VMEM((PIECES, rows, piece), bf16),
            pltpu.VMEM((8, rows), f32),
            pltpu.VMEM((8, rows), f32),
            pltpu.VMEM((2, 2, rows, ep_size // 2 * cap), bf16),
            pltpu.VMEM((max(8, ep_size), rows), f32),
            pltpu.VMEM((rows, width), bf16),
            dma((9,)),
            dma((2,)),
            dma,
            dma((blocks,)),
            dma,
            dma((2,)),
            dma,
            dma((blocks,)),
            dma,
            dma((2,)),
            dma,
            dma((PIECES, 2)),
            dma,
            dma,
            dma((3,)),
            dma((3,)),
            dma,
            dma((PIECES,)),
            dma,
            dma,
            dma,
            dma,
        ],
        compiler_params=pltpu.CompilerParams(
            collective_id=0, has_side_effects=True, vmem_limit_bytes=62 * 1024 * 1024
        ),
    )(
        expert_input,
        norm_gain.reshape(1, width),
        conv_taps,
        expert_ids.T,
        route_weight.T,
        out_gate,
        in_gate,
        conv_input,
        mixer_weight,
        expert_gate[0],
        expert_up[0],
        expert_down[0],
    )
    held = [pltpu.with_memory_space_constraint(a, pltpu.VMEM) for a in (mix, out)]
    return placed(*held)


def solution(mesh):
    ep_size, tp_size = mesh.shape["ep"], mesh.shape["tp"]
    body = fused if tp_size == 4 and ep_size <= 8 else local
    return jax.shard_map(
        body,
        mesh=mesh,
        in_specs=(
            P(("ep", "tp"), None),
            P(("ep", "tp"), None),
            P(("ep", "tp"), None),
            P(),
            P(None, "tp"),
            P(("ep", "tp"), None),
            P(),
            P("ep", None, "tp"),
            P("ep", None, "tp"),
            P("ep", "tp", None),
            P(("ep", "tp"), None),
            P(("ep", "tp"), None),
        ),
        out_specs=(P("ep", "tp"), P(("ep", "tp"), None)),
        check_vma=False,
    )
```

```python
import functools

import jax
import jax.numpy as jnp
from jax import lax
from jax.experimental import pallas as pl
from jax.experimental.pallas import tpu as pltpu
from jax.sharding import PartitionSpec as P

CONV = 3
SEQS = 1


norm_eps = 1e-06


def from_behind(value, axis, steps):
    count = lax.axis_size(axis)
    first, last = (max(0, -steps), min(count, count - steps))
    return lax.ppermute(value, axis, [(source, source + steps) for source in range(first, last)])


def device_slots(route_ids, expert_count):
    flat_ids = route_ids.reshape(-1)
    member = (flat_ids[:, None] == jnp.arange(expert_count, dtype=jnp.int32)[None, :]).astype(
        jnp.int32
    )
    before = jnp.cumsum(member, axis=0) - member
    return jnp.sum(before * member, axis=1).reshape(route_ids.shape)


def fill_slots(row_data, route_ids, expert_count, slot_cap):
    top_count = route_ids.shape[1]
    position = (route_ids * slot_cap + device_slots(route_ids, expert_count)).reshape(-1)
    zeroed = jnp.zeros((expert_count * slot_cap, row_data.shape[1]), row_data.dtype)
    return zeroed.at[position].set(jnp.repeat(row_data, top_count, axis=0))


def expert_hidden(slot_rows, w_gate, w_up):
    gate_proj = jnp.dot(slot_rows, w_gate, preferred_element_type=jnp.float32)
    up_proj = jnp.dot(slot_rows, w_up, preferred_element_type=jnp.float32)
    return (jax.nn.silu(gate_proj) * up_proj).astype(jnp.bfloat16)


def local(
    out_gate,
    in_gate,
    conv_input,
    conv_taps,
    mixer_weight,
    expert_input,
    norm_gain,
    expert_gate,
    expert_up,
    expert_down,
    expert_ids,
    route_weight,
):
    row_count = in_gate.shape[0]
    tap_span = CONV - 1
    group_size = lax.axis_size("tp")
    product = in_gate.astype(jnp.float32) * conv_input.astype(jnp.float32)
    edge_product = from_behind(product[row_count - tap_span :], ("ep", "tp"), 1)
    seq_length = row_count * lax.axis_size("ep") * group_size // SEQS
    linear_index = lax.axis_index("ep") * group_size + lax.axis_index("tp")
    carry_over = jnp.where(linear_index * row_count % seq_length == 0, 0.0, 1.0).astype(jnp.float32)
    earlier = edge_product * carry_over
    padded = jnp.concatenate([earlier, product], axis=0)
    tap_values = conv_taps.astype(jnp.float32)
    smoothed = sum(
        (
            padded[tap_index : tap_index + row_count] * tap_values[tap_index]
            for tap_index in range(CONV)
        )
    )
    gated = (out_gate.astype(jnp.float32) * smoothed).astype(jnp.bfloat16)
    token_count = expert_input.shape[0]
    model_width = expert_input.shape[1]
    expert_count = lax.axis_size("ep")
    slot_cap = 4 * token_count // expert_count
    wide_input = expert_input.astype(jnp.float32)
    inv_norm = lax.rsqrt(jnp.mean(wide_input * wide_input, axis=1, keepdims=True) + norm_eps)
    normed = (wide_input * inv_norm * norm_gain).astype(jnp.bfloat16)
    w_gate = expert_gate[0]
    hidden_width = w_gate.shape[1]
    position = (expert_ids * slot_cap + device_slots(expert_ids, expert_count)).reshape(-1)
    whole_gate, whole_up, whole_down = (
        lax.all_gather(expert_gate, "tp", axis=2, tiled=True),
        lax.all_gather(expert_up, "tp", axis=2, tiled=True),
        lax.all_gather(expert_down, "tp", axis=1, tiled=True),
    )
    mixer_out = jnp.dot(
        lax.all_gather(gated, "tp", axis=0, tiled=True),
        mixer_weight,
        preferred_element_type=jnp.float32,
    ).astype(jnp.bfloat16)
    outgoing = fill_slots(normed, expert_ids, expert_count, slot_cap).reshape(
        expert_count, slot_cap, model_width
    )
    arrived = lax.all_to_all(outgoing, "ep", split_axis=0, concat_axis=0, tiled=True)
    hidden = expert_hidden(arrived.reshape(-1, model_width), whole_gate[0], whole_up[0])
    running = jnp.zeros((hidden.shape[0], model_width), jnp.float32)
    for quarter in range(group_size):
        partial_sum = jnp.dot(
            hidden[:, quarter * hidden_width : (quarter + 1) * hidden_width],
            whole_down[0, quarter * hidden_width : (quarter + 1) * hidden_width],
            preferred_element_type=jnp.float32,
        )
        running = running + lax.optimization_barrier(partial_sum.astype(jnp.bfloat16)).astype(
            jnp.float32
        )
    summed = running.astype(jnp.bfloat16)
    returned = lax.all_to_all(
        summed.reshape(expert_count, slot_cap, model_width),
        "ep",
        split_axis=0,
        concat_axis=0,
        tiled=True,
    )
    picked = returned.reshape(expert_count * slot_cap, model_width)[position]
    top_count = expert_ids.shape[1]
    picked = picked.reshape(token_count, top_count, model_width).astype(jnp.float32)
    route_share = route_weight / jnp.sum(route_weight, axis=1, keepdims=True)
    experts_out = jnp.sum(picked * route_share[:, :, None], axis=1).astype(jnp.bfloat16)
    return (mixer_out, experts_out)


MESH = pl.DeviceIdType.MESH
SHARES = (1,1,2,2,2,2,2,2,2)
PIECES = len(SHARES)
SPLITS = 8
EAGER = 4
AHEAD = 6
FIRST = 6
SOON = 2
BEHIND = 2


def fused_kernel(
    ep_size,
    tp_size,
    cap,
    x_hbm,
    gain_hbm,
    taps_hbm,
    ids_hbm,
    weight_hbm,
    og_hbm,
    ig_hbm,
    ci_hbm,
    mw_hbm,
    wg_hbm,
    wu_hbm,
    wd_hbm,
    mix_ref,
    out_ref,
    x_ref,
    gain_ref,
    taps_ref,
    ids_ref,
    weight_ref,
    og,
    ig,
    ci,
    mw,
    gates,
    ups,
    downs,
    xs,
    xr,
    hid,
    g_sum,
    u_sum,
    ys,
    yr,
    yf,
    prod,
    gat,
    place,
    normed,
    summed,
    sums,
    info,
    their_info,
    picks,
    far_picks,
    half_sums,
    share,
    their_place,
    their_rows,
    bypass,
    local_sem,
    own_sem,
    y_send,
    y_recv,
    c_send,
    c_recv,
    f_send,
    f_recv,
    x_send,
    x_recv,
    r_send,
    r_recv,
    e_send,
    e_recv,
    g_send,
    g_recv,
    p_send,
    p_recv,
    m_send,
    m_recv,
    n_send,
    n_recv,
    v_send,
    v_recv,
    i_send,
    q_recv,
):
    f32, bf16 = jnp.float32, jnp.bfloat16
    ep, tp = lax.axis_index("ep"), lax.axis_index("tp")
    rows, width = x_ref.shape
    x_copies, og_copies = (2, 3, 4, 7), (5, 6)
    unit = width // sum(SHARES)
    spans = [(sum(SHARES[:j]) * unit, SHARES[j] * unit) for j in range(PIECES)]
    cols = [pl.ds(*span) for span in spans]
    depth = width // SPLITS
    part = wd_hbm.shape[0]
    tp_c = tp + 1 - 2 * lax.rem(tp, 2)
    tp_y = lax.rem(tp + 2, tp_size)
    line = ep * tp_size + tp
    count = ep_size * tp_size
    after, before = lax.rem(line + 1, count), lax.rem(line + count - 1, count)
    after_id = (after // tp_size, lax.rem(after, tp_size))
    before_id = (before // tp_size, lax.rem(before, tp_size))
    core_id, y_id = (ep, tp_c), (ep, tp_y)

    bits = [1 << b for b in range(ep_size.bit_length() - 1)]
    half = ep_size // 2

    def peer(k):
        return sum(lax.rem(ep // b + k // b, 2) * b for b in bits)

    pair = half // 2
    near = ep // half
    far = 1 - near
    inner = lax.rem((ep // pair + 1) // 2, 2)
    is_inner, is_outer = inner == 1, inner == 0
    behind = (peer(half + pair), peer(half))
    across = inner * behind[0] + (1 - inner) * behind[1]
    barrier = pltpu.get_barrier_semaphore()
    partners = [(peer(k), tp) for k in range(1, half + 1)] + [core_id, y_id, after_id, before_id]
    partners.append((peer(pair), tp_y))
    for partner in partners:
        pl.semaphore_signal(barrier, inc=1, device_id=partner, device_id_type=MESH)

    @pl.when(is_inner)
    def _():
        pl.semaphore_signal(barrier, inc=1, device_id=(behind[0], tp), device_id_type=MESH)


    stage = [
        pltpu.make_async_copy(s, d, local_sem.at[i])
        for i, (s, d) in enumerate(
            (
                (ig_hbm, ig),
                (ci_hbm, ci),
                (x_hbm, x_ref),
                (ids_hbm, ids_ref),
                (gain_hbm, gain_ref),
                (og_hbm, og),
                (taps_hbm, taps_ref),
                (weight_hbm, weight_ref),
                (mw_hbm, mw),
            )
        )
    ]
    for copy in stage:
        copy.start()

    def parts(owner):
        cut = [(wg_hbm, gates.at[owner])]
        for k in range(SPLITS):
            deep = pl.ds(k * depth, depth)
            cut.append((wu_hbm.at[deep], ups.at[owner, deep]))
        at = pl.ds(pl.multiple_of(owner * part, part), part)
        for j in range(PIECES):
            cut.append((wd_hbm.at[:, cols[j]], downs.at[at, cols[j]]))
        return cut

    def remote(s, d, ss, rs, who):
        return pltpu.make_async_remote_copy(
            src_ref=s, dst_ref=d, send_sem=ss, recv_sem=rs, device_id=who, device_id_type=MESH
        )

    def taken(ref, sem):
        pltpu.make_async_copy(ref, ref, sem).wait()

    group = [0] * (1 + SPLITS) + [1] * PIECES
    held = (gates.at[0:2], gates.at[0])
    own = [pltpu.make_async_copy(s, d, own_sem.at[g]) for g, (s, d) in zip(group, parts(tp))]
    for copy in own:
        copy.start()
    head = 8
    strip = 256
    stage[0].wait()
    stage[1].wait()
    last = slice(rows - head, rows)
    prod[rows : rows + head, :] = ig[last, :].astype(f32) * ci[last, :].astype(f32)
    edge = remote(prod.at[rows : rows + head], prod.at[0:head], e_send, e_recv, after_id)
    to_y = [remote(s, d, y_send, y_recv.at[i], y_id) for i, (s, d) in enumerate(parts(tp))]
    to_c = [remote(s, d, c_send, c_recv.at[g], core_id) for g, (s, d) in zip(group, parts(tp))]
    pl.semaphore_wait(barrier, len(partners) + inner)
    edge.start()
    around = remote(parts(tp)[1][0], bypass, y_send, v_recv, (peer(pair), tp_y))
    to_y[0].start()
    pl.when(is_inner)(to_y[1].start)
    pl.when(is_outer)(around.start)
    for copy in to_y[2:] + to_c:
        copy.start()

    def multiply(i, carry):
        c = pl.ds(pl.multiple_of(i * strip, strip), strip)
        first = slice(0, rows - head)
        prod[head:rows, c] = ig[first, c].astype(f32) * ci[first, c].astype(f32)
        return carry

    lax.fori_loop(0, width // strip, multiply, 0)

    for i in x_copies:
        stage[i].wait()
    ids_row = ids_ref[...]
    info[...] = jnp.concatenate(
        [ids_row.astype(f32), weight_ref[...], jnp.zeros((4, rows), f32)], axis=0
    )
    to_set = 1 - inner
    tell = remote(info, their_info.at[to_set], m_send, m_recv.at[to_set], (across, tp))
    tell.start()
    lanes = place.shape[1]
    ti = lax.broadcasted_iota(jnp.int32, (rows, rows), 0)
    tj = lax.broadcasted_iota(jnp.int32, (rows, rows), 1)
    upper = jnp.where(ti < tj, 1.0, 0.0).astype(bf16)
    expert_row = lax.broadcasted_iota(jnp.int32, place.shape, 0).astype(f32)

    def rank_rows(source, target):
        member = (source[0:1, :] == expert_row) | (source[1:2, :] == expert_row)
        member = jnp.where(member, 1.0, 0.0)
        rank = jnp.dot(member.astype(bf16), upper, preferred_element_type=f32)
        target[...] = jnp.where(member > 0.5, rank, -1.0)

    rank_rows(info, place)
    wide = x_ref[...].astype(f32)
    inv = lax.rsqrt(jnp.mean(wide * wide, axis=1, keepdims=True) + norm_eps)
    normed[...] = (wide * inv * gain_ref[...]).astype(bf16)
    slot = lax.broadcasted_iota(jnp.int32, (cap, rows), 0).astype(f32)
    across_rows = remote(normed, their_rows.at[to_set], n_send, n_recv.at[to_set], (across, tp))
    pl.when(is_inner)(across_rows.start)

    def chosen(e, places, source):
        pick = jnp.where(places[pl.ds(e, 1), :] == slot, 1.0, 0.0).astype(bf16)
        return jnp.dot(pick, source[...], preferred_element_type=f32).astype(bf16)

    def send_rows(places, source, t, origin, which):
        def body(i, carry):
            e = peer(2 - i + 3 * (i // 2))
            at = (t - near) * half + e
            xs[at] = chosen(e, places, source)
            remote(xs.at[at], xr.at[origin], x_send, x_recv.at[which], (e, tp)).start()
            return carry

        lax.fori_loop(0, half - 1, body, 0)
        xr[origin] = chosen(ep, places, source)

    send_rows(place, normed, 0, ep, 0)

    for i in og_copies:
        stage[i].wait()
    edge.wait_recv()

    @pl.when(line * rows % (rows * count // SEQS) == 0)
    def _():
        prod[0:head, :] = jnp.zeros((head, width), f32)

    def smooth(i, carry):
        c = pl.ds(pl.multiple_of(i * strip, strip), strip)
        taps = taps_ref[:, c].astype(f32)
        total = prod[head : head + rows, c] * taps[CONV - 1 : CONV]
        for j in range(CONV - 1):
            lo = head - (CONV - 1) + j
            total = total + prod[lo : lo + rows, c] * taps[j : j + 1]
        gat[tp, :, c] = (og[:, c].astype(f32) * total).astype(bf16)
        return carry

    lax.fori_loop(0, width // strip, smooth, 0)
    g_y = remote(gat.at[tp], gat.at[tp], g_send.at[0], g_recv.at[0], y_id)
    g_c = remote(gat.at[tp], gat.at[tp], g_send.at[1], g_recv.at[1], core_id)
    g_y.start()
    g_c.start()

    def mix(t):
        mix_ref[pl.ds(pl.multiple_of(t * rows, rows), rows), :] = jnp.dot(
            gat[t], mw[...], preferred_element_type=f32
        ).astype(bf16)

    stage[8].wait()
    g_c.wait_recv()

    def mix_two(i, carry):
        mix(2 * (tp // 2) + i)
        return carry

    lax.fori_loop(0, 2, mix_two, 0)
    pl.when(is_outer)(across_rows.start)

    lane = tj.astype(f32)
    lower = jnp.where(tj < ti, 1.0, 0.0).astype(bf16)
    def column(row):
        return jnp.sum(jnp.where(ti == tj, row, 0.0), axis=1, keepdims=True)

    def route(source, first, target, portion):
        named = [column(source[k : k + 1, :]) for k in range(2)]
        weight = [column(source[2 + k : 3 + k, :]) for k in range(2)]
        member = jnp.where((named[0] == lane) | (named[1] == lane), 1.0, 0.0).astype(bf16)
        ranks = jnp.dot(lower, member, preferred_element_type=f32)
        slots = lax.broadcasted_iota(jnp.int32, target.shape[1:], 1).astype(f32)
        for k in range(2):
            rank = jnp.sum(jnp.where(lane == named[k], ranks, 0.0), axis=1, keepdims=True)
            at = (named[k] - first.astype(f32)) * cap + rank
            target[k] = jnp.where(slots == at, 1.0, 0.0).astype(bf16)
            portion[k] = weight[k] / (weight[0] + weight[1])

    route(info, near * half, picks, share.at[0])

    def weighted(blocks, j, table, portion):
        block = blocks[:, :, cols[j]].reshape(table.shape[2], spans[j][1])
        total = portion[0] * jnp.dot(table[0], block, preferred_element_type=f32)
        return total + portion[1] * jnp.dot(table[1], block, preferred_element_type=f32)

    def learn(t):
        taken(their_info.at[t], m_recv.at[t])
        route(their_info.at[t], ep // pair * pair, far_picks.at[t], share.at[1 + t])

    @pl.when(is_inner)
    def _():
        for t in range(2):
            learn(t)
            remote(
                their_info.at[t], their_info.at[t], i_send, m_recv.at[t], (peer(pair), tp)
            ).start()
            rank_rows(their_info.at[t], their_place.at[t])
            taken(their_rows.at[t], n_recv.at[t])
            send_rows(their_place.at[t], their_rows.at[t], 1 + t, behind[t], 1)
            if t == 0:
                taken(bypass, v_recv)
                deep = pl.ds(0, depth)
                remote(
                    bypass, ups.at[tp_y, deep], v_send, y_recv.at[1], (peer(pair), tp)
                ).start()

    dest_y = parts(tp_y)
    forward = [
        remote(d, d, f_send, f_recv.at[i], core_id) for i, (_, d) in enumerate(dest_y)
    ]

    def side_rows(side):
        return pl.ds(pl.multiple_of(side * (half * cap), half * cap), half * cap)

    def units(q):
        return pl.ds(pl.multiple_of(q * part, part), part)

    def gated_units(g, u):
        return (g / (1.0 + jnp.exp(-g)) * u).astype(bf16)

    def arrived(side):
        return xr[pl.ds(side * half, half)].reshape(half * cap, width)

    def hidden(q, side):
        x = arrived(side)
        g = jnp.dot(x, gates[q], preferred_element_type=f32)
        u = jnp.dot(x, ups[q], preferred_element_type=f32)
        hid[side_rows(side), units(q)] = gated_units(g, u)

    chip, chip_other = 2 * (tp // 2), 1 - 2 * lax.rem(tp, 2)
    taken(xr.at[0 : half - 1], x_recv.at[0])
    taken(held[0], own_sem.at[0])
    taken(held[0], c_recv.at[0])

    crossed = (tp_y, tp_y + chip_other)

    def own_units(side):
        def body(i, carry):
            hidden(chip + i, side)
            return carry

        lax.fori_loop(0, 2, body, 0)

    def gate_part(i, side):
        g_sum[i, side_rows(side), :] = jnp.dot(
            arrived(side), gates[crossed[i]], preferred_element_type=f32
        )

    def up_part(i, k, side, count=1):
        deep = slice(k * depth, (k + count) * depth)
        at = side_rows(side)
        x = xr[pl.ds(side * half, half), :, deep].reshape(half * cap, count * depth)
        u = jnp.dot(x, ups[crossed[i], deep], preferred_element_type=f32)
        if k:
            u = u + u_sum[i, at, :]
        if k + count < SPLITS:
            u_sum[i, at, :] = u
        else:
            hid[at, units(crossed[i])] = gated_units(g_sum[i, at, :], u)

    def up_both(i, k):
        def body(side, carry):
            up_part(i, k, side)
            return carry

        lax.fori_loop(0, 2, body, 0)

    own_units(near)

    @pl.when(is_outer)
    def _():
        for t in range(2):
            learn(t)

    to_y[0].wait_recv()
    forward[0].start()
    gate_part(0, near)
    forward[0].wait_recv()
    gate_part(1, near)
    for k in range(AHEAD):
        to_y[1 + k].wait_recv()
        forward[1 + k].start()
        up_part(0, k, near)
        forward[1 + k].wait_recv()
        up_part(1, k, near)
    pl.when(is_inner)(functools.partial(taken, xr.at[0:pair], x_recv.at[1]))
    pl.when(is_outer)(functools.partial(taken, xr.at[0:half], x_recv.at[1]))
    own_units(far)
    for i in range(2):
        gate_part(i, far)
        up_part(i, 0, far, AHEAD)
    for k in range(AHEAD, SPLITS):
        to_y[1 + k].wait_recv()
        forward[1 + k].start()
        if k > AHEAD:
            forward[k].wait_recv()
            up_both(1, k - 1)
        up_both(0, k)
    to_y[1 + SPLITS].wait_recv()
    forward[1 + SPLITS].start()
    forward[SPLITS].wait_recv()
    up_both(1, SPLITS - 1)

    mine = ep - near * half

    own_column = lax.rem(ep, pair)
    other_column = 1 - own_column

    def send_near(j):
        for k in (pair, 1, half - 1):
            s = peer(k)
            remote(
                ys.at[s, :, cols[j]], yr.at[mine, :, cols[j]], r_send, r_recv.at[j, 0], (s, tp)
            ).start()

    def far_of(t, column):
        return ((2 - near) if t == 0 else (3 - 3 * near)) * pair + column

    def send_far(j):
        for t in range(2):
            remote(
                ys.at[far_of(t, other_column), :, cols[j]],
                yf.at[t, own_column, :, cols[j]],
                r_send,
                r_recv.at[j, 1],
                (peer(1), tp),
            ).start()
            yf[t, own_column, :, cols[j]] = ys[far_of(t, own_column), :, cols[j]]

    def collect(j, t):
        return weighted(yf.at[t], j, far_picks.at[t], share.at[1 + t])

    def pass_on(j):
        @pl.when(is_outer)
        def _():
            taken(yf.at[:, 0, :, cols[j]], r_recv.at[j, 1])
            for t in range(2):
                summed[t, :, cols[j]] = collect(j, t).astype(bf16)
            remote(
                summed.at[:, :, cols[j]],
                half_sums.at[:, :, cols[j]],
                p_send,
                q_recv.at[j],
                (peer(pair), tp),
            ).start()

    def relay(j):
        @pl.when(is_inner)
        def _():
            taken(yf.at[:, 0, :, cols[j]], r_recv.at[j, 1])
            taken(half_sums.at[:, :, cols[j]], q_recv.at[j])
            for t in range(2):
                total = collect(j, t) + half_sums[t, :, cols[j]].astype(f32)
                summed[t, :, cols[j]] = total.astype(bf16)
                remote(
                    summed.at[t, :, cols[j]],
                    sums.at[:, cols[j]],
                    p_send,
                    p_recv.at[j],
                    (behind[t], tp),
                ).start()

    def down(j, side):
        total = jnp.dot(hid[side_rows(side), :], downs[:, cols[j]], preferred_element_type=f32)
        ys[pl.ds(side * half, half), :, cols[j]] = total.astype(bf16).reshape(
            half, cap, spans[j][1]
        )

    def finish(j):
        taken(yr.at[0 : half - 1, :, cols[j]], r_recv.at[j, 0])
        taken(sums.at[:, cols[j]], p_recv.at[j])
        total = weighted(yr, j, picks, share.at[0]) + sums[:, cols[j]].astype(f32)
        out_ref[:, cols[j]] = total.astype(bf16)

    taken(held[1], own_sem.at[1])
    taken(held[1], c_recv.at[1])
    for j in range(PIECES):
        m = 1 + SPLITS + j
        if j:
            to_y[m].wait_recv()
            forward[m].start()
        if j >= SOON:
            pass_on(j - SOON)
        if j >= BEHIND:
            relay(j - BEHIND)
        forward[m].wait_recv()
        down(j, far)
        send_far(j)
        down(j, near)
        yr[mine, :, cols[j]] = ys[ep, :, cols[j]]
        if j < EAGER:
            send_near(j)
        else:
            pl.when(is_inner)(functools.partial(send_near, j))

    for j in range(PIECES - SOON, PIECES):
        pass_on(j)

    @pl.when(is_outer)
    def _():
        for j in range(EAGER, PIECES):
            send_near(j)

    for j in range(PIECES - BEHIND, PIECES):
        relay(j)

    for j in range(FIRST):
        finish(j)

    g_y.wait_recv()
    g_f = remote(gat.at[tp_y], gat.at[tp_y], g_send.at[2], g_recv.at[2], core_id)
    g_f.start()
    mix(tp_y)
    for j in range(FIRST, PIECES - 1):
        finish(j)
    g_f.wait_recv()
    mix(tp_y + chip_other)
    for j in range(PIECES - 1, PIECES):
        finish(j)

    for sem in (y_send, c_send, f_send):
        taken(gates.at[0:3], sem)
    taken(xr.at[0 : half - 1], x_send)
    taken(xr.at[0 : half + 1], r_send)
    taken(summed, p_send)
    for copy in [g_y, g_c, g_f, tell, across_rows, edge]:
        copy.wait_send()

    @pl.when(is_inner)
    def _():
        taken(xr.at[0 : 2 * (half - 1)], x_send)
        taken(their_info, i_send)
        taken(bypass, v_send)


def place_kernel(mix_ref, out_ref, mix_hbm, out_hbm, sem):
    copies = [
        pltpu.make_async_copy(mix_ref, mix_hbm, sem.at[0]),
        pltpu.make_async_copy(out_ref, out_hbm, sem.at[1]),
    ]
    for copy in copies:
        copy.start()
    for copy in copies:
        copy.wait()


def placed(mix, out):
    vmem, hbm = pl.BlockSpec(memory_space=pltpu.VMEM), pl.BlockSpec(memory_space=pltpu.HBM)
    return pl.pallas_call(
        place_kernel,
        out_shape=tuple(jax.ShapeDtypeStruct(a.shape, a.dtype) for a in (mix, out)),
        in_specs=[vmem, vmem],
        out_specs=(hbm, hbm),
        scratch_shapes=[pltpu.SemaphoreType.DMA((2,))],
    )(mix, out)


def fused(
    out_gate,
    in_gate,
    conv_input,
    conv_taps,
    mixer_weight,
    expert_input,
    norm_gain,
    expert_gate,
    expert_up,
    expert_down,
    expert_ids,
    route_weight,
):
    ep_size, tp_size = lax.axis_size("ep"), lax.axis_size("tp")
    rows, width = expert_input.shape
    cap = 4 * rows // ep_size
    part = expert_gate.shape[2]
    columns = mixer_weight.shape[1]
    bf16, f32 = jnp.bfloat16, jnp.float32
    vmem, hbm = pl.BlockSpec(memory_space=pltpu.VMEM), pl.BlockSpec(memory_space=pltpu.HBM)
    dma = pltpu.SemaphoreType.DMA
    blocks = 1 + SPLITS + PIECES
    mix, out = pl.pallas_call(
        functools.partial(fused_kernel, ep_size, tp_size, cap),
        out_shape=(
            pltpu.VMEM((rows * tp_size, columns), bf16),
            pltpu.VMEM((rows, width), bf16),
        ),
        in_specs=[hbm] * 12,
        out_specs=(vmem, vmem),
        scratch_shapes=[
            pltpu.VMEM((rows, width), bf16),
            pltpu.VMEM((1, width), f32),
            pltpu.VMEM(conv_taps.shape, bf16),
            pltpu.VMEM((expert_ids.shape[1], rows), jnp.int32),
            pltpu.VMEM((expert_ids.shape[1], rows), f32),
            pltpu.VMEM((rows, width), bf16),
            pltpu.VMEM((rows, width), bf16),
            pltpu.VMEM((rows, width), bf16),
            pltpu.VMEM(mixer_weight.shape, bf16),
            pltpu.VMEM((tp_size, width, part), bf16),
            pltpu.VMEM((tp_size, width, part), bf16),
            pltpu.VMEM((tp_size * part, width), bf16),
            pltpu.VMEM((ep_size // 2 * 3, cap, width), bf16),
            pltpu.VMEM((ep_size, cap, width), bf16),
            pltpu.VMEM((ep_size * cap, tp_size * part), bf16),
            pltpu.VMEM((2, ep_size * cap, part), f32),
            pltpu.VMEM((2, ep_size * cap, part), f32),
            pltpu.VMEM((ep_size, cap, width), bf16),
            pltpu.VMEM((ep_size // 2, cap, width), bf16),
            pltpu.VMEM((2, ep_size // 4, cap, width), bf16),
            pltpu.VMEM((rows + 8, width), f32),
            pltpu.VMEM((tp_size, rows, width), bf16),
            pltpu.VMEM((max(8, ep_size), rows), f32),
            pltpu.VMEM((rows, width), bf16),
            pltpu.VMEM((2, rows, width), bf16),
            pltpu.VMEM((rows, width), bf16),
            pltpu.VMEM((8, rows), f32),
            pltpu.VMEM((2, 8, rows), f32),
            pltpu.VMEM((2, rows, ep_size // 2 * cap), bf16),
            pltpu.VMEM((2, 2, rows, ep_size // 4 * cap), bf16),
            pltpu.VMEM((2, rows, width), bf16),
            pltpu.VMEM((3, 2, rows, 1), f32),
            pltpu.VMEM((2, max(8, ep_size), rows), f32),
            pltpu.VMEM((2, rows, width), bf16),
            pltpu.VMEM((width // SPLITS, part), bf16),
            dma((9,)),
            dma((2,)),
            dma,
            dma((blocks,)),
            dma,
            dma((2,)),
            dma,
            dma((blocks,)),
            dma,
            dma((2,)),
            dma,
            dma((PIECES, 2)),
            dma,
            dma,
            dma((3,)),
            dma((3,)),
            dma,
            dma((PIECES,)),
            dma,
            dma((2,)),
            dma,
            dma((2,)),
            dma,
            dma,
            dma,
            dma((PIECES,)),
        ],
        compiler_params=pltpu.CompilerParams(
            collective_id=0, has_side_effects=True, vmem_limit_bytes=62 * 1024 * 1024
        ),
    )(
        expert_input,
        norm_gain.reshape(1, width),
        conv_taps,
        expert_ids.T,
        route_weight.T,
        out_gate,
        in_gate,
        conv_input,
        mixer_weight,
        expert_gate[0],
        expert_up[0],
        expert_down[0],
    )
    held = [pltpu.with_memory_space_constraint(a, pltpu.VMEM) for a in (mix, out)]
    return placed(*held)


def solution(mesh):
    ep_size, tp_size = mesh.shape["ep"], mesh.shape["tp"]
    body = fused if tp_size == 4 and ep_size == 8 else local
    return jax.shard_map(
        body,
        mesh=mesh,
        in_specs=(
            P(("ep", "tp"), None),
            P(("ep", "tp"), None),
            P(("ep", "tp"), None),
            P(),
            P(None, "tp"),
            P(("ep", "tp"), None),
            P(),
            P("ep", None, "tp"),
            P("ep", None, "tp"),
            P("ep", "tp", None),
            P(("ep", "tp"), None),
            P(("ep", "tp"), None),
        ),
        out_specs=(P("ep", "tp"), P(("ep", "tp"), None)),
        check_vma=False,
    )
```

```python
import functools

import jax
import jax.numpy as jnp
from jax import lax
from jax.experimental import pallas as pl
from jax.experimental.pallas import tpu as pltpu
from jax.sharding import PartitionSpec as P

CONV = 3
SEQS = 1


norm_eps = 1e-06


def from_behind(value, axis, steps):
    count = lax.axis_size(axis)
    first, last = (max(0, -steps), min(count, count - steps))
    return lax.ppermute(value, axis, [(source, source + steps) for source in range(first, last)])


def device_slots(route_ids, expert_count):
    flat_ids = route_ids.reshape(-1)
    member = (flat_ids[:, None] == jnp.arange(expert_count, dtype=jnp.int32)[None, :]).astype(
        jnp.int32
    )
    before = jnp.cumsum(member, axis=0) - member
    return jnp.sum(before * member, axis=1).reshape(route_ids.shape)


def fill_slots(row_data, route_ids, expert_count, slot_cap):
    top_count = route_ids.shape[1]
    position = (route_ids * slot_cap + device_slots(route_ids, expert_count)).reshape(-1)
    zeroed = jnp.zeros((expert_count * slot_cap, row_data.shape[1]), row_data.dtype)
    return zeroed.at[position].set(jnp.repeat(row_data, top_count, axis=0))


def expert_hidden(slot_rows, w_gate, w_up):
    gate_proj = jnp.dot(slot_rows, w_gate, preferred_element_type=jnp.float32)
    up_proj = jnp.dot(slot_rows, w_up, preferred_element_type=jnp.float32)
    return (jax.nn.silu(gate_proj) * up_proj).astype(jnp.bfloat16)


def local(
    out_gate,
    in_gate,
    conv_input,
    conv_taps,
    mixer_weight,
    expert_input,
    norm_gain,
    expert_gate,
    expert_up,
    expert_down,
    expert_ids,
    route_weight,
):
    row_count = in_gate.shape[0]
    tap_span = CONV - 1
    group_size = lax.axis_size("tp")
    product = in_gate.astype(jnp.float32) * conv_input.astype(jnp.float32)
    edge_product = from_behind(product[row_count - tap_span :], ("ep", "tp"), 1)
    seq_length = row_count * lax.axis_size("ep") * group_size // SEQS
    linear_index = lax.axis_index("ep") * group_size + lax.axis_index("tp")
    carry_over = jnp.where(linear_index * row_count % seq_length == 0, 0.0, 1.0).astype(jnp.float32)
    earlier = edge_product * carry_over
    padded = jnp.concatenate([earlier, product], axis=0)
    tap_values = conv_taps.astype(jnp.float32)
    smoothed = sum(
        (
            padded[tap_index : tap_index + row_count] * tap_values[tap_index]
            for tap_index in range(CONV)
        )
    )
    gated = (out_gate.astype(jnp.float32) * smoothed).astype(jnp.bfloat16)
    token_count = expert_input.shape[0]
    model_width = expert_input.shape[1]
    expert_count = lax.axis_size("ep")
    slot_cap = 4 * token_count // expert_count
    wide_input = expert_input.astype(jnp.float32)
    inv_norm = lax.rsqrt(jnp.mean(wide_input * wide_input, axis=1, keepdims=True) + norm_eps)
    normed = (wide_input * inv_norm * norm_gain).astype(jnp.bfloat16)
    w_gate = expert_gate[0]
    hidden_width = w_gate.shape[1]
    position = (expert_ids * slot_cap + device_slots(expert_ids, expert_count)).reshape(-1)
    whole_gate, whole_up, whole_down = (
        lax.all_gather(expert_gate, "tp", axis=2, tiled=True),
        lax.all_gather(expert_up, "tp", axis=2, tiled=True),
        lax.all_gather(expert_down, "tp", axis=1, tiled=True),
    )
    mixer_out = jnp.dot(
        lax.all_gather(gated, "tp", axis=0, tiled=True),
        mixer_weight,
        preferred_element_type=jnp.float32,
    ).astype(jnp.bfloat16)
    outgoing = fill_slots(normed, expert_ids, expert_count, slot_cap).reshape(
        expert_count, slot_cap, model_width
    )
    arrived = lax.all_to_all(outgoing, "ep", split_axis=0, concat_axis=0, tiled=True)
    hidden = expert_hidden(arrived.reshape(-1, model_width), whole_gate[0], whole_up[0])
    running = jnp.zeros((hidden.shape[0], model_width), jnp.float32)
    for quarter in range(group_size):
        partial_sum = jnp.dot(
            hidden[:, quarter * hidden_width : (quarter + 1) * hidden_width],
            whole_down[0, quarter * hidden_width : (quarter + 1) * hidden_width],
            preferred_element_type=jnp.float32,
        )
        running = running + lax.optimization_barrier(partial_sum.astype(jnp.bfloat16)).astype(
            jnp.float32
        )
    summed = running.astype(jnp.bfloat16)
    returned = lax.all_to_all(
        summed.reshape(expert_count, slot_cap, model_width),
        "ep",
        split_axis=0,
        concat_axis=0,
        tiled=True,
    )
    picked = returned.reshape(expert_count * slot_cap, model_width)[position]
    top_count = expert_ids.shape[1]
    picked = picked.reshape(token_count, top_count, model_width).astype(jnp.float32)
    route_share = route_weight / jnp.sum(route_weight, axis=1, keepdims=True)
    experts_out = jnp.sum(picked * route_share[:, :, None], axis=1).astype(jnp.bfloat16)
    return (mixer_out, experts_out)


MESH = pl.DeviceIdType.MESH
SHARES = (1,1,2,2,2,2,2,2,2)
PIECES = len(SHARES)
DEEPS = (1, 4, 1, 1, 1)
SPLITS = len(DEEPS)
EAGER = 4
AHEAD = 2
FIRST = 6
SOON = 2
BEHIND = 2


def fused_kernel(
    ep_size,
    tp_size,
    cap,
    x_hbm,
    gain_hbm,
    taps_hbm,
    ids_hbm,
    weight_hbm,
    og_hbm,
    ig_hbm,
    ci_hbm,
    mw_hbm,
    wg_hbm,
    wu_hbm,
    wd_hbm,
    mix_ref,
    out_ref,
    x_ref,
    gain_ref,
    taps_ref,
    ids_ref,
    weight_ref,
    og,
    ig,
    ci,
    mw,
    gates,
    ups,
    downs,
    xs,
    xr,
    hid,
    g_sum,
    u_sum,
    ys,
    yr,
    yf,
    prod,
    gat,
    place,
    normed,
    summed,
    sums,
    info,
    their_info,
    picks,
    far_picks,
    half_sums,
    share,
    their_place,
    their_rows,
    bypass,
    local_sem,
    own_sem,
    y_send,
    y_recv,
    c_send,
    c_recv,
    f_send,
    f_recv,
    x_send,
    x_recv,
    r_send,
    r_recv,
    e_send,
    e_recv,
    g_send,
    g_recv,
    p_send,
    p_recv,
    m_send,
    m_recv,
    n_send,
    n_recv,
    v_send,
    v_recv,
    i_send,
    q_recv,
):
    f32, bf16 = jnp.float32, jnp.bfloat16
    ep, tp = lax.axis_index("ep"), lax.axis_index("tp")
    rows, width = x_ref.shape
    x_copies, og_copies = (2, 3, 4, 7), (5, 6)
    unit = width // sum(SHARES)
    spans = [(sum(SHARES[:j]) * unit, SHARES[j] * unit) for j in range(PIECES)]
    cols = [pl.ds(*span) for span in spans]
    depth = width // sum(DEEPS)
    edges = [sum(DEEPS[:k]) * depth for k in range(SPLITS + 1)]
    part = wd_hbm.shape[0]
    tp_c = tp + 1 - 2 * lax.rem(tp, 2)
    tp_y = lax.rem(tp + 2, tp_size)
    line = ep * tp_size + tp
    count = ep_size * tp_size
    after, before = lax.rem(line + 1, count), lax.rem(line + count - 1, count)
    after_id = (after // tp_size, lax.rem(after, tp_size))
    before_id = (before // tp_size, lax.rem(before, tp_size))
    core_id, y_id = (ep, tp_c), (ep, tp_y)

    bits = [1 << b for b in range(ep_size.bit_length() - 1)]
    half = ep_size // 2

    def peer(k):
        return sum(lax.rem(ep // b + k // b, 2) * b for b in bits)

    pair = half // 2
    near = ep // half
    far = 1 - near
    inner = lax.rem((ep // pair + 1) // 2, 2)
    is_inner, is_outer = inner == 1, inner == 0
    behind = (peer(half + pair), peer(half))
    across = inner * behind[0] + (1 - inner) * behind[1]
    barrier = pltpu.get_barrier_semaphore()
    partners = [(peer(k), tp) for k in range(1, half + 1)] + [core_id, y_id, after_id, before_id]
    partners.append((peer(pair), tp_y))
    for partner in partners:
        pl.semaphore_signal(barrier, inc=1, device_id=partner, device_id_type=MESH)

    @pl.when(is_inner)
    def _():
        pl.semaphore_signal(barrier, inc=1, device_id=(behind[0], tp), device_id_type=MESH)


    stage = [
        pltpu.make_async_copy(s, d, local_sem.at[i])
        for i, (s, d) in enumerate(
            (
                (ig_hbm, ig),
                (ci_hbm, ci),
                (x_hbm, x_ref),
                (ids_hbm, ids_ref),
                (gain_hbm, gain_ref),
                (og_hbm, og),
                (taps_hbm, taps_ref),
                (weight_hbm, weight_ref),
                (mw_hbm, mw),
            )
        )
    ]
    for copy in stage:
        copy.start()

    def parts(owner):
        cut = [(wg_hbm, gates.at[owner])]
        for k in range(SPLITS):
            deep = pl.ds(edges[k], edges[k + 1] - edges[k])
            cut.append((wu_hbm.at[deep], ups.at[owner, deep]))
        at = pl.ds(pl.multiple_of(owner * part, part), part)
        for j in range(PIECES):
            cut.append((wd_hbm.at[:, cols[j]], downs.at[at, cols[j]]))
        return cut

    def remote(s, d, ss, rs, who):
        return pltpu.make_async_remote_copy(
            src_ref=s, dst_ref=d, send_sem=ss, recv_sem=rs, device_id=who, device_id_type=MESH
        )

    def taken(ref, sem):
        pltpu.make_async_copy(ref, ref, sem).wait()

    group = [0] * (1 + SPLITS) + [1] * PIECES
    held = (gates.at[0:2], gates.at[0])
    own = [pltpu.make_async_copy(s, d, own_sem.at[g]) for g, (s, d) in zip(group, parts(tp))]
    for copy in own:
        copy.start()
    head = 8
    strip = 256
    stage[0].wait()
    stage[1].wait()
    last = slice(rows - head, rows)
    prod[rows : rows + head, :] = ig[last, :].astype(f32) * ci[last, :].astype(f32)
    edge = remote(prod.at[rows : rows + head], prod.at[0:head], e_send, e_recv, after_id)
    to_y = [remote(s, d, y_send, y_recv.at[i], y_id) for i, (s, d) in enumerate(parts(tp))]
    to_c = [remote(s, d, c_send, c_recv.at[g], core_id) for g, (s, d) in zip(group, parts(tp))]
    pl.semaphore_wait(barrier, len(partners) + inner)
    edge.start()
    around = remote(parts(tp)[1][0], bypass, y_send, v_recv, (peer(pair), tp_y))
    to_y[0].start()
    pl.when(is_inner)(to_y[1].start)
    pl.when(is_outer)(around.start)
    for copy in to_y[2:] + to_c:
        copy.start()

    def multiply(i, carry):
        c = pl.ds(pl.multiple_of(i * strip, strip), strip)
        first = slice(0, rows - head)
        prod[head:rows, c] = ig[first, c].astype(f32) * ci[first, c].astype(f32)
        return carry

    lax.fori_loop(0, width // strip, multiply, 0)

    for i in x_copies:
        stage[i].wait()
    ids_row = ids_ref[...]
    info[...] = jnp.concatenate(
        [ids_row.astype(f32), weight_ref[...], jnp.zeros((4, rows), f32)], axis=0
    )
    to_set = 1 - inner
    tell = remote(info, their_info.at[to_set], m_send, m_recv.at[to_set], (across, tp))
    tell.start()
    lanes = place.shape[1]
    ti = lax.broadcasted_iota(jnp.int32, (rows, rows), 0)
    tj = lax.broadcasted_iota(jnp.int32, (rows, rows), 1)
    upper = jnp.where(ti < tj, 1.0, 0.0).astype(bf16)
    expert_row = lax.broadcasted_iota(jnp.int32, place.shape, 0).astype(f32)

    def rank_rows(source, target):
        member = (source[0:1, :] == expert_row) | (source[1:2, :] == expert_row)
        member = jnp.where(member, 1.0, 0.0)
        rank = jnp.dot(member.astype(bf16), upper, preferred_element_type=f32)
        target[...] = jnp.where(member > 0.5, rank, -1.0)

    rank_rows(info, place)
    wide = x_ref[...].astype(f32)
    inv = lax.rsqrt(jnp.mean(wide * wide, axis=1, keepdims=True) + norm_eps)
    normed[...] = (wide * inv * gain_ref[...]).astype(bf16)
    slot = lax.broadcasted_iota(jnp.int32, (cap, rows), 0).astype(f32)
    across_rows = remote(normed, their_rows.at[to_set], n_send, n_recv.at[to_set], (across, tp))
    pl.when(is_inner)(across_rows.start)

    def chosen(e, places, source):
        pick = jnp.where(places[pl.ds(e, 1), :] == slot, 1.0, 0.0).astype(bf16)
        return jnp.dot(pick, source[...], preferred_element_type=f32).astype(bf16)

    def send_rows(places, source, t, origin, which):
        def body(i, carry):
            e = peer(2 - i + 3 * (i // 2))
            at = (t - near) * half + e
            xs[at] = chosen(e, places, source)
            remote(xs.at[at], xr.at[origin], x_send, x_recv.at[which], (e, tp)).start()
            return carry

        lax.fori_loop(0, half - 1, body, 0)
        xr[origin] = chosen(ep, places, source)

    send_rows(place, normed, 0, ep, 0)

    for i in og_copies:
        stage[i].wait()
    edge.wait_recv()

    @pl.when(line * rows % (rows * count // SEQS) == 0)
    def _():
        prod[0:head, :] = jnp.zeros((head, width), f32)

    def smooth(i, carry):
        c = pl.ds(pl.multiple_of(i * strip, strip), strip)
        taps = taps_ref[:, c].astype(f32)
        total = prod[head : head + rows, c] * taps[CONV - 1 : CONV]
        for j in range(CONV - 1):
            lo = head - (CONV - 1) + j
            total = total + prod[lo : lo + rows, c] * taps[j : j + 1]
        gat[tp, :, c] = (og[:, c].astype(f32) * total).astype(bf16)
        return carry

    lax.fori_loop(0, width // strip, smooth, 0)
    halves = [pl.ds(h * (rows // 2), rows // 2) for h in range(2)]
    g_y = [
        remote(gat.at[tp, h], gat.at[tp, h], g_send.at[0], g_recv.at[2 * n], y_id)
        for n, h in enumerate(halves)
    ]
    g_c = remote(gat.at[tp], gat.at[tp], g_send.at[1], g_recv.at[1], core_id)
    g_c.start()
    for copy in g_y:
        copy.start()

    def mix(t):
        mix_ref[pl.ds(pl.multiple_of(t * rows, rows), rows), :] = jnp.dot(
            gat[t], mw[...], preferred_element_type=f32
        ).astype(bf16)

    stage[8].wait()
    g_c.wait_recv()

    def mix_two(i, carry):
        mix(2 * (tp // 2) + i)
        return carry

    lax.fori_loop(0, 2, mix_two, 0)
    pl.when(is_outer)(across_rows.start)

    lane = tj.astype(f32)
    lower = jnp.where(tj < ti, 1.0, 0.0).astype(bf16)
    def column(row):
        return jnp.sum(jnp.where(ti == tj, row, 0.0), axis=1, keepdims=True)

    def route(source, first, target, portion):
        named = [column(source[k : k + 1, :]) for k in range(2)]
        weight = [column(source[2 + k : 3 + k, :]) for k in range(2)]
        member = jnp.where((named[0] == lane) | (named[1] == lane), 1.0, 0.0).astype(bf16)
        ranks = jnp.dot(lower, member, preferred_element_type=f32)
        slots = lax.broadcasted_iota(jnp.int32, target.shape[1:], 1).astype(f32)
        for k in range(2):
            rank = jnp.sum(jnp.where(lane == named[k], ranks, 0.0), axis=1, keepdims=True)
            at = (named[k] - first.astype(f32)) * cap + rank
            target[k] = jnp.where(slots == at, 1.0, 0.0).astype(bf16)
            portion[k] = weight[k] / (weight[0] + weight[1])

    route(info, near * half, picks, share.at[0])

    def weighted(blocks, j, table, portion):
        block = blocks[:, :, cols[j]].reshape(table.shape[2], spans[j][1])
        total = portion[0] * jnp.dot(table[0], block, preferred_element_type=f32)
        return total + portion[1] * jnp.dot(table[1], block, preferred_element_type=f32)

    def learn(t):
        taken(their_info.at[t], m_recv.at[t])
        route(their_info.at[t], ep // pair * pair, far_picks.at[t], share.at[1 + t])

    @pl.when(is_inner)
    def _():
        for t in range(2):
            learn(t)
            remote(
                their_info.at[t], their_info.at[t], i_send, m_recv.at[t], (peer(pair), tp)
            ).start()
            rank_rows(their_info.at[t], their_place.at[t])
            taken(their_rows.at[t], n_recv.at[t])
            send_rows(their_place.at[t], their_rows.at[t], 1 + t, behind[t], 1)
            if t == 0:
                taken(bypass, v_recv)
                deep = pl.ds(0, depth)
                remote(
                    bypass, ups.at[tp_y, deep], v_send, y_recv.at[1], (peer(pair), tp)
                ).start()

    dest_y = parts(tp_y)
    forward = [
        remote(d, d, f_send, f_recv.at[i], core_id) for i, (_, d) in enumerate(dest_y)
    ]

    def side_rows(side):
        return pl.ds(pl.multiple_of(side * (half * cap), half * cap), half * cap)

    def units(q):
        return pl.ds(pl.multiple_of(q * part, part), part)

    def gated_units(g, u):
        return (g / (1.0 + jnp.exp(-g)) * u).astype(bf16)

    def arrived(side):
        return xr[pl.ds(side * half, half)].reshape(half * cap, width)

    def hidden(q, side):
        x = arrived(side)
        g = jnp.dot(x, gates[q], preferred_element_type=f32)
        u = jnp.dot(x, ups[q], preferred_element_type=f32)
        hid[side_rows(side), units(q)] = gated_units(g, u)

    chip, chip_other = 2 * (tp // 2), 1 - 2 * lax.rem(tp, 2)
    taken(xr.at[0 : half - 1], x_recv.at[0])
    taken(held[0], own_sem.at[0])
    taken(held[0], c_recv.at[0])

    crossed = (tp_y, tp_y + chip_other)

    def own_units(side):
        def body(i, carry):
            hidden(chip + i, side)
            return carry

        lax.fori_loop(0, 2, body, 0)

    def gate_part(i, side):
        g_sum[i, side_rows(side), :] = jnp.dot(
            arrived(side), gates[crossed[i]], preferred_element_type=f32
        )

    def up_part(i, k, side, count=1):
        deep = slice(edges[k], edges[k + count])
        at = side_rows(side)
        x = xr[pl.ds(side * half, half), :, deep].reshape(half * cap, edges[k + count] - edges[k])
        u = jnp.dot(x, ups[crossed[i], deep], preferred_element_type=f32)
        if k:
            u = u + u_sum[i, at, :]
        if k + count < SPLITS:
            u_sum[i, at, :] = u
        else:
            hid[at, units(crossed[i])] = gated_units(g_sum[i, at, :], u)

    def up_both(i, k):
        def body(side, carry):
            up_part(i, k, side)
            return carry

        lax.fori_loop(0, 2, body, 0)

    own_units(near)

    @pl.when(is_outer)
    def _():
        for t in range(2):
            learn(t)

    to_y[0].wait_recv()
    forward[0].start()
    gate_part(0, near)
    forward[0].wait_recv()
    gate_part(1, near)
    for k in range(AHEAD):
        to_y[1 + k].wait_recv()
        forward[1 + k].start()
        up_part(0, k, near)
        forward[1 + k].wait_recv()
        up_part(1, k, near)
    pl.when(is_inner)(functools.partial(taken, xr.at[0:pair], x_recv.at[1]))
    pl.when(is_outer)(functools.partial(taken, xr.at[0:half], x_recv.at[1]))
    own_units(far)
    for i in range(2):
        gate_part(i, far)
        up_part(i, 0, far, AHEAD)
    for k in range(AHEAD, SPLITS):
        to_y[1 + k].wait_recv()
        forward[1 + k].start()
        if k > AHEAD:
            forward[k].wait_recv()
            up_both(1, k - 1)
        up_both(0, k)
    to_y[1 + SPLITS].wait_recv()
    forward[1 + SPLITS].start()
    forward[SPLITS].wait_recv()
    up_both(1, SPLITS - 1)

    mine = ep - near * half

    own_column = lax.rem(ep, pair)
    other_column = 1 - own_column

    def send_near(j):
        for k in (pair, 1, half - 1):
            s = peer(k)
            remote(
                ys.at[s, :, cols[j]], yr.at[mine, :, cols[j]], r_send, r_recv.at[j, 0], (s, tp)
            ).start()

    def far_of(t, column):
        return ((2 - near) if t == 0 else (3 - 3 * near)) * pair + column

    def send_far(j):
        for t in range(2):
            remote(
                ys.at[far_of(t, other_column), :, cols[j]],
                yf.at[t, own_column, :, cols[j]],
                r_send,
                r_recv.at[j, 1],
                (peer(1), tp),
            ).start()
            yf[t, own_column, :, cols[j]] = ys[far_of(t, own_column), :, cols[j]]

    def collect(j, t):
        return weighted(yf.at[t], j, far_picks.at[t], share.at[1 + t])

    def pass_on(j):
        @pl.when(is_outer)
        def _():
            taken(yf.at[:, 0, :, cols[j]], r_recv.at[j, 1])
            for t in range(2):
                summed[t, :, cols[j]] = collect(j, t).astype(bf16)
            remote(
                summed.at[:, :, cols[j]],
                half_sums.at[:, :, cols[j]],
                p_send,
                q_recv.at[j],
                (peer(pair), tp),
            ).start()

    def relay(j):
        @pl.when(is_inner)
        def _():
            taken(yf.at[:, 0, :, cols[j]], r_recv.at[j, 1])
            taken(half_sums.at[:, :, cols[j]], q_recv.at[j])
            for t in range(2):
                total = collect(j, t) + half_sums[t, :, cols[j]].astype(f32)
                summed[t, :, cols[j]] = total.astype(bf16)
                remote(
                    summed.at[t, :, cols[j]],
                    sums.at[:, cols[j]],
                    p_send,
                    p_recv.at[j],
                    (behind[t], tp),
                ).start()

    def down(j, side):
        total = jnp.dot(hid[side_rows(side), :], downs[:, cols[j]], preferred_element_type=f32)
        ys[pl.ds(side * half, half), :, cols[j]] = total.astype(bf16).reshape(
            half, cap, spans[j][1]
        )

    def finish(j):
        taken(yr.at[0 : half - 1, :, cols[j]], r_recv.at[j, 0])
        taken(sums.at[:, cols[j]], p_recv.at[j])
        total = weighted(yr, j, picks, share.at[0]) + sums[:, cols[j]].astype(f32)
        out_ref[:, cols[j]] = total.astype(bf16)

    taken(held[1], own_sem.at[1])
    taken(held[1], c_recv.at[1])
    for j in range(PIECES):
        m = 1 + SPLITS + j
        if j:
            to_y[m].wait_recv()
            forward[m].start()
        if j >= SOON:
            pass_on(j - SOON)
        if j >= BEHIND:
            relay(j - BEHIND)
        forward[m].wait_recv()
        down(j, far)
        send_far(j)
        down(j, near)
        yr[mine, :, cols[j]] = ys[ep, :, cols[j]]
        if j < EAGER:
            send_near(j)
        else:
            pl.when(is_inner)(functools.partial(send_near, j))

    for j in range(PIECES - SOON, PIECES):
        pass_on(j)

    @pl.when(is_outer)
    def _():
        for j in range(EAGER, PIECES):
            send_near(j)

    for j in range(PIECES - BEHIND, PIECES):
        relay(j)

    for j in range(FIRST):
        finish(j)

    g_f = [
        remote(gat.at[tp_y, h], gat.at[tp_y, h], g_send.at[2], g_recv.at[3 + n], core_id)
        for n, h in enumerate(halves)
    ]
    for n in range(2):
        g_y[n].wait_recv()
        g_f[n].start()
    mix(tp_y)
    for j in range(FIRST, PIECES - 1):
        finish(j)
    for copy in g_f:
        copy.wait_recv()
    mix(tp_y + chip_other)
    for j in range(PIECES - 1, PIECES):
        finish(j)

    for sem in (y_send, c_send, f_send):
        taken(gates.at[0:3], sem)
    taken(xr.at[0 : half - 1], x_send)
    taken(xr.at[0 : half + 1], r_send)
    taken(summed, p_send)
    taken(gat.at[0], g_send.at[0])
    taken(gat.at[0], g_send.at[2])
    for copy in [g_c, tell, across_rows, edge]:
        copy.wait_send()

    @pl.when(is_inner)
    def _():
        taken(xr.at[0 : 2 * (half - 1)], x_send)
        taken(their_info, i_send)
        taken(bypass, v_send)


def place_kernel(mix_ref, out_ref, mix_hbm, out_hbm, sem):
    copies = [
        pltpu.make_async_copy(mix_ref, mix_hbm, sem.at[0]),
        pltpu.make_async_copy(out_ref, out_hbm, sem.at[1]),
    ]
    for copy in copies:
        copy.start()
    for copy in copies:
        copy.wait()


def placed(mix, out):
    vmem, hbm = pl.BlockSpec(memory_space=pltpu.VMEM), pl.BlockSpec(memory_space=pltpu.HBM)
    return pl.pallas_call(
        place_kernel,
        out_shape=tuple(jax.ShapeDtypeStruct(a.shape, a.dtype) for a in (mix, out)),
        in_specs=[vmem, vmem],
        out_specs=(hbm, hbm),
        scratch_shapes=[pltpu.SemaphoreType.DMA((2,))],
    )(mix, out)


def fused(
    out_gate,
    in_gate,
    conv_input,
    conv_taps,
    mixer_weight,
    expert_input,
    norm_gain,
    expert_gate,
    expert_up,
    expert_down,
    expert_ids,
    route_weight,
):
    ep_size, tp_size = lax.axis_size("ep"), lax.axis_size("tp")
    rows, width = expert_input.shape
    cap = 4 * rows // ep_size
    part = expert_gate.shape[2]
    columns = mixer_weight.shape[1]
    bf16, f32 = jnp.bfloat16, jnp.float32
    vmem, hbm = pl.BlockSpec(memory_space=pltpu.VMEM), pl.BlockSpec(memory_space=pltpu.HBM)
    dma = pltpu.SemaphoreType.DMA
    blocks = 1 + SPLITS + PIECES
    mix, out = pl.pallas_call(
        functools.partial(fused_kernel, ep_size, tp_size, cap),
        out_shape=(
            pltpu.VMEM((rows * tp_size, columns), bf16),
            pltpu.VMEM((rows, width), bf16),
        ),
        in_specs=[hbm] * 12,
        out_specs=(vmem, vmem),
        scratch_shapes=[
            pltpu.VMEM((rows, width), bf16),
            pltpu.VMEM((1, width), f32),
            pltpu.VMEM(conv_taps.shape, bf16),
            pltpu.VMEM((expert_ids.shape[1], rows), jnp.int32),
            pltpu.VMEM((expert_ids.shape[1], rows), f32),
            pltpu.VMEM((rows, width), bf16),
            pltpu.VMEM((rows, width), bf16),
            pltpu.VMEM((rows, width), bf16),
            pltpu.VMEM(mixer_weight.shape, bf16),
            pltpu.VMEM((tp_size, width, part), bf16),
            pltpu.VMEM((tp_size, width, part), bf16),
            pltpu.VMEM((tp_size * part, width), bf16),
            pltpu.VMEM((ep_size // 2 * 3, cap, width), bf16),
            pltpu.VMEM((ep_size, cap, width), bf16),
            pltpu.VMEM((ep_size * cap, tp_size * part), bf16),
            pltpu.VMEM((2, ep_size * cap, part), f32),
            pltpu.VMEM((2, ep_size * cap, part), f32),
            pltpu.VMEM((ep_size, cap, width), bf16),
            pltpu.VMEM((ep_size // 2, cap, width), bf16),
            pltpu.VMEM((2, ep_size // 4, cap, width), bf16),
            pltpu.VMEM((rows + 8, width), f32),
            pltpu.VMEM((tp_size, rows, width), bf16),
            pltpu.VMEM((max(8, ep_size), rows), f32),
            pltpu.VMEM((rows, width), bf16),
            pltpu.VMEM((2, rows, width), bf16),
            pltpu.VMEM((rows, width), bf16),
            pltpu.VMEM((8, rows), f32),
            pltpu.VMEM((2, 8, rows), f32),
            pltpu.VMEM((2, rows, ep_size // 2 * cap), bf16),
            pltpu.VMEM((2, 2, rows, ep_size // 4 * cap), bf16),
            pltpu.VMEM((2, rows, width), bf16),
            pltpu.VMEM((3, 2, rows, 1), f32),
            pltpu.VMEM((2, max(8, ep_size), rows), f32),
            pltpu.VMEM((2, rows, width), bf16),
            pltpu.VMEM((width // sum(DEEPS), part), bf16),
            dma((9,)),
            dma((2,)),
            dma,
            dma((blocks,)),
            dma,
            dma((2,)),
            dma,
            dma((blocks,)),
            dma,
            dma((2,)),
            dma,
            dma((PIECES, 2)),
            dma,
            dma,
            dma((3,)),
            dma((5,)),
            dma,
            dma((PIECES,)),
            dma,
            dma((2,)),
            dma,
            dma((2,)),
            dma,
            dma,
            dma,
            dma((PIECES,)),
        ],
        compiler_params=pltpu.CompilerParams(
            collective_id=0, has_side_effects=True, vmem_limit_bytes=62 * 1024 * 1024
        ),
    )(
        expert_input,
        norm_gain.reshape(1, width),
        conv_taps,
        expert_ids.T,
        route_weight.T,
        out_gate,
        in_gate,
        conv_input,
        mixer_weight,
        expert_gate[0],
        expert_up[0],
        expert_down[0],
    )
    held = [pltpu.with_memory_space_constraint(a, pltpu.VMEM) for a in (mix, out)]
    return placed(*held)


def solution(mesh):
    ep_size, tp_size = mesh.shape["ep"], mesh.shape["tp"]
    body = fused if tp_size == 4 and ep_size == 8 else local
    return jax.shard_map(
        body,
        mesh=mesh,
        in_specs=(
            P(("ep", "tp"), None),
            P(("ep", "tp"), None),
            P(("ep", "tp"), None),
            P(),
            P(None, "tp"),
            P(("ep", "tp"), None),
            P(),
            P("ep", None, "tp"),
            P("ep", None, "tp"),
            P("ep", "tp", None),
            P(("ep", "tp"), None),
            P(("ep", "tp"), None),
        ),
        out_specs=(P("ep", "tp"), P(("ep", "tp"), None)),
        check_vma=False,
    )
```
